32 devices in a mesh: ep: 16 (over z, y, core), tp: 2 (over x).
Axes of the slice: x: 2, y: 2, z: 4, core: 2. Of those that a mesh axis runs over, the one named last changes fastest.
Arguments:
- tokens: bfloat16 [128, 1024], P(('ep', 'tp')), may hold values from -6 to 6
- lengths: int32 [128], P('ep'), may hold values from 256 to 1024
- key_cache: bfloat16 [128, 1024, 128], P(('ep', 'tp')), may hold values from -1500 to 1500
- value_cache: bfloat16 [128, 1024, 128], P(('ep', 'tp')), may hold values from -6 to 6
- query_weight: bfloat16 [1024, 512], P(None, 'tp'), may hold values from -0.1875 to 0.1875
- key_weight: bfloat16 [1024, 128], replicated, may hold values from -0.1875 to 0.1875
- value_weight: bfloat16 [1024, 128], replicated, may hold values from -0.1875 to 0.1875
- lambdas: float32 [4], replicated, may hold values from 0.3 to 0.8
- head_gain: float32 [128], replicated, may hold values from 0.1 to 1.9
- output_weight: bfloat16 [512, 1024], P(None, 'tp'), may hold values from -0.25 to 0.25
- norm1_gain: float32 [1024], replicated, may hold values from 0.1 to 1.9
- routes: int32 [128, 6], P('ep'), may hold values from 0 to 15, all different within a row; in each aligned block of 8 rows (0 to 7, 8 to 15, ...) at most 6 rows name the same one
- route_logits: float32 [128, 6], P('ep'), may hold values from -9 to 410
- gate_weight: bfloat16 [16, 1024, 1024], P('ep', None, 'tp'), may hold values from -0.5 to 0.5
- up_weight: bfloat16 [16, 1024, 1024], P('ep', None, 'tp'), may hold values from -0.5 to 0.5
- down_weight: bfloat16 [16, 1024, 1024], P('ep', 'tp'), may hold values from -0.09375 to 0.09375
- norm2_gain: float32 [1024], replicated, may hold values from 0.1 to 1.9
Outputs:
- mixed: bfloat16 [128, 1024], P('ep', 'tp')
The draws below stay inside these ranges and needn't reach their ends.
Inputs may be any that keep to these rules, and one draw needn't show every extreme that they name: `routes`: in the 8 rows of each aligned block (the rows held by one index of ep) no expert is named by more than 6 rows, a bound that some block reaches; the experts of a row differ.
All inputs are finite; a program needn't handle non-finite values.
Results may differ from the reference program's by a relative error of at most 0.014.
Values may be sent and summed in bfloat16 or wider, within the bound.
A program may use at most 64 MiB of HBM per device.

```python
import math
import jax
import jax.numpy as jnp
import numpy as np
from jax import lax

D = 1024
HEADS = 4
DH = 64
VH = 128
FF = 1024
TOPK = 6
CACHE = 1024
TOK_GRP = 8
BATCH = 128
EXPERTS = 16
CAP = 6
N_EP = 16
N_TP = 2


def draw_key_cache(key, part):
    base = jnp.clip(jax.random.normal(key, (BATCH, CACHE, 2 * DH), jnp.float32) * 1.75, -9.0, 9.0)
    return base.astype(jnp.bfloat16)


def draw_route_logits(key, part):
    base = jnp.clip(jax.random.normal(key, (BATCH, TOPK), jnp.float32) * 1.5, -9.0, 9.0)
    return base


def touch_ends(values, key, smallest, top_value):
    index_at = [jax.random.randint(jax.random.fold_in(key, axis), (), 0, length) for axis, length in enumerate(values.shape)]
    longest = values.shape.index(max(values.shape))
    neighbour = index_at[:longest] + [(index_at[longest] + 1) % values.shape[longest]] + index_at[longest + 1:]
    return values.at[tuple(index_at)].set(smallest).at[tuple(neighbour)].set(top_value)


def block_levels(key, extent, cuts, least, largest):
    level = 1.0
    for axis_at, parts in cuts:
        heights = jax.random.uniform(jax.random.fold_in(jax.random.fold_in(key, 6), axis_at), (parts,), jnp.float32, least / len(cuts), largest / len(cuts))
        level = level * jnp.repeat(jnp.exp(heights), extent[axis_at] // parts).reshape((-1,) + (1,) * (len(extent) - 1 - axis_at))
    return level


def deal_out(own_key, own, number, rows, amount, top, bound, lean):
    sequence = jax.random.permutation(own_key, amount)
    heavy_load, ordinary = load_shares(amount, rows * top, bound, lean, True), load_shares(amount, rows * top, bound, lean, False)
    places = jnp.arange(amount)

    def named(sizes, rotation):
        used = int((sizes > 0).sum())
        fixed = max(1, used // 4)
        moved = fixed + (places - fixed + rotation * (used - fixed)) % max(1, amount - fixed)
        return jnp.zeros((amount,), jnp.int32).at[sequence[jnp.where(places < fixed, places, moved)]].set(jnp.asarray(sizes, jnp.int32))

    sizes = jnp.where(number % 4 == 0, named(heavy_load, number // 4), named(ordinary, number - number // 4 - 1))
    mixed = jax.random.permutation(jax.random.fold_in(own, 3), amount)
    source_of, receiver = mixed[0:amount // 2 * 2:2], mixed[1:amount // 2 * 2:2]
    room = jnp.minimum(sizes[source_of] - 1, bound - sizes[receiver]) // 2
    room = jnp.where((source_of == sequence[0]) | (receiver == sequence[0]) | (sizes[receiver] == 0), 0, jnp.maximum(room, 0))
    moved = jax.random.randint(jax.random.fold_in(own, 4), (amount // 2,), 0, 1 << 20) % (room + 1)
    sizes = sizes.at[source_of].add(-moved).at[receiver].add(moved)
    members = jnp.searchsorted(jnp.cumsum(sizes), jnp.arange(rows * top), side="right").astype(jnp.int32)
    grid = members.reshape(top, rows).T
    grid = grid[jax.random.permutation(jax.random.fold_in(own, 1), rows)]
    rotation = jax.random.randint(jax.random.fold_in(own, 2), (rows, 1), 0, top)
    return jnp.take_along_axis(grid, (jnp.arange(top)[None, :] + rotation) % top, axis=1)


def load_shares(number_of, total, reach, skew, full):
    weights = [(1 << 20) // math.isqrt(grade ** skew) + 1 for grade in range(1, number_of + 1)]
    largest = reach if full else min(reach, max(-(-total // number_of), total * weights[0] // sum(weights)))
    least = 1 if total - largest >= number_of - 1 else 0
    given, rest = [largest] + [least] * (number_of - 1), total - largest - least * (number_of - 1)
    while rest > 0:
        candidates = [i for i in range(1, number_of) if given[i] < largest] or [i for i in range(1, number_of) if given[i] < reach]
        whole, budget = sum([weights[i] for i in candidates]), rest
        for i in candidates:
            more = min(reach - given[i], max(1, budget * weights[i] // whole), rest)
            given[i] = given[i] + more
            rest = rest - more
    return np.array(given)


def gaussian(key, shape, scale, most, cuts=(), kind=jnp.bfloat16):
    entries = jax.random.normal(key, shape, jnp.float32) * scale
    if len(cuts) > 0:
        entries = block_levels(key, shape, cuts, -0.22, 0.18) * entries
    return jnp.clip(entries, min=-most, max=most).astype(kind)


def setup_inputs(seed: int = 0) -> dict:
    key_list = jax.random.split(jax.random.key(seed), 18)
    tokens = gaussian(key_list[0], (BATCH, D), 1.0, 6.0, ((0, 32),))
    lengths = touch_ends(jax.random.randint(key_list[1], (BATCH,), CACHE // 4, CACHE + 1), jax.random.fold_in(key_list[1], 1), CACHE // 4, CACHE).astype(jnp.int32)
    key_cache = draw_key_cache(jax.random.fold_in(key_list[17], 71), 0)
    value_cache = gaussian(key_list[3], (BATCH, CACHE, VH), 1.0, 6.0, ((0, 32),))
    query_weight = gaussian(key_list[4], (D, 2 * DH * HEADS), D ** -0.5, 0.1875, ((1, 2),))
    key_weight = gaussian(key_list[5], (D, 2 * DH), D ** -0.5, 0.1875)
    value_weight = gaussian(key_list[6], (D, VH), D ** -0.5, 0.1875)
    lambdas = jnp.clip(jax.random.uniform(key_list[7], (HEADS,), jnp.float32, 0.3, 0.8), 0.3, 0.8)
    head_gain = jnp.clip(1.0 + 0.18 * jax.random.normal(key_list[8], (VH,), jnp.float32), 0.1, 1.9)
    output_weight = gaussian(key_list[9], (HEADS * VH, D), (HEADS * VH) ** -0.5, 0.25, ((1, 2),))
    norm1_gain = jnp.clip(1.0 + 0.18 * jax.random.normal(key_list[10], (D,), jnp.float32), 0.1, 1.9)
    routes_keys = jax.random.split(jax.random.fold_in(key_list[11], 1), BATCH // TOK_GRP)
    routes_turns = jax.random.permutation(jax.random.fold_in(key_list[11], 3), BATCH // TOK_GRP)
    routes = jax.vmap(lambda own, number: deal_out(jax.random.fold_in(key_list[11], 2), own, number, TOK_GRP, EXPERTS, TOPK, CAP, 2))(routes_keys, routes_turns).reshape((BATCH, TOPK))
    route_logits = draw_route_logits(jax.random.fold_in(key_list[17], 71), 0)
    gate_weight = gaussian(key_list[13], (EXPERTS, D, FF), (D // 9) ** -0.5, 0.5, ((0, 16), (2, 2)))
    up_weight = gaussian(key_list[14], (EXPERTS, D, FF), (D // 9) ** -0.5, 0.5, ((0, 16), (2, 2)))
    down_weight = gaussian(key_list[15], (EXPERTS, FF, D), (4 * FF) ** -0.5, 0.09375, ((0, 16), (1, 2)))
    norm2_gain = jnp.clip(1.0 + 0.18 * jax.random.normal(key_list[16], (D,), jnp.float32), 0.1, 1.9)
    return {"tokens": tokens, "lengths": lengths, "key_cache": key_cache, "value_cache": value_cache, "query_weight": query_weight, "key_weight": key_weight, "value_weight": value_weight, "lambdas": lambdas, "head_gain": head_gain, "output_weight": output_weight, "norm1_gain": norm1_gain, "routes": routes, "route_logits": route_logits, "gate_weight": gate_weight, "up_weight": up_weight, "down_weight": down_weight, "norm2_gain": norm2_gain}


ALPHA = 1.4142135623730951
EPS = 1e-05
THETA = 500000.0
LIMIT = 7.0
SLOPE = 1.702

def rotate(values, positions):
    half = values.shape[-1] // 2
    freqs = THETA ** (-jnp.arange(half, dtype=jnp.float32) / half)
    angles = positions.astype(jnp.float32)[:, None] * freqs[None, :]
    shape = (angles.shape[0],) + (1,) * (values.ndim - 2) + (half,)
    cosine = jnp.cos(angles).reshape(shape)
    sine = jnp.sin(angles).reshape(shape)
    first = values[..., :half]
    second = values[..., half:]
    return jnp.concatenate([first * cosine - second * sine, second * cosine + first * sine], axis=-1)

def norm_rows(summed, gain):
    mean = lax.optimization_barrier(jnp.mean(summed, axis=-1, keepdims=True))
    center = summed - mean
    spread = lax.optimization_barrier(jnp.mean(center * center, axis=-1, keepdims=True))
    return center * lax.rsqrt(spread + EPS) * gain

def choose_slots(routes_block, experts, capacity):
    flat = routes_block.reshape(-1).astype(jnp.int32)
    onehot = (flat[:, None] == jnp.arange(experts, dtype=jnp.int32)[None, :]).astype(jnp.int32)
    before = jnp.cumsum(onehot, axis=0) - onehot
    slot = lax.optimization_barrier(jnp.sum(before * onehot, axis=1))
    target = flat * capacity + slot
    return target[:, None] == jnp.arange(experts * capacity, dtype=jnp.int32)[None, :]

def attend_block(query, new_key, new_value, keys, values, lengths, lambdas, head_gain):
    f32 = jnp.float32
    count, length = (keys.shape[0], keys.shape[1])
    keys = keys.reshape(count, length, 2, -1)
    scale = keys.shape[-1] ** (-0.5)
    past = jnp.einsum('bhmd,bjmd->bhmj', query.astype(f32), keys.astype(f32)) * scale
    live = jnp.arange(length, dtype=jnp.int32)[None, :] < lengths[:, None]
    past = jnp.where(live[:, None, None, :], past, -jnp.inf)
    selfs = jnp.einsum('bhmd,bmd->bhm', query.astype(f32), new_key.astype(f32)) * scale
    top = jnp.maximum(lax.optimization_barrier(jnp.max(past, axis=-1)), selfs)
    past_exp = jnp.exp(past - top[..., None])
    self_exp = jnp.exp(selfs - top)
    total = lax.optimization_barrier(jnp.sum(past_exp, axis=-1)) + self_exp
    past_prob = past_exp / total[..., None]
    self_prob = self_exp / total
    mixing = lambdas[None, :]
    past_weight = (past_prob[:, :, 0] - mixing[..., None] * past_prob[:, :, 1]).astype(jnp.bfloat16)
    self_weight = (self_prob[:, :, 0] - mixing * self_prob[:, :, 1]).astype(jnp.bfloat16)
    head_out = jnp.einsum('bhj,bje->bhe', past_weight.astype(f32), values.astype(f32))
    head_out = head_out + self_weight.astype(f32)[..., None] * new_value.astype(f32)[:, None, :]
    normed = head_out * lax.rsqrt(lax.optimization_barrier(jnp.mean(head_out * head_out, axis=-1, keepdims=True)) + EPS) * head_gain
    return normed.astype(jnp.bfloat16).reshape(count, -1)

def reference(tokens, lengths, key_cache, value_cache, query_weight, key_weight, value_weight, lambdas, head_gain, output_weight, norm1_gain, routes, route_logits, gate_weight, up_weight, down_weight, norm2_gain):
    f32 = jnp.float32
    bf16 = jnp.bfloat16
    rows = tokens.shape[0]
    query = jnp.dot(tokens, query_weight, preferred_element_type=f32).reshape(rows, HEADS, 2, DH)
    query = rotate(query, lengths).astype(bf16)
    new_key = jnp.dot(tokens, key_weight, preferred_element_type=f32).reshape(rows, 2, DH)
    new_key = rotate(new_key, lengths).astype(bf16)
    new_value = jnp.dot(tokens, value_weight, preferred_element_type=f32).astype(bf16)

    def one_group(pieces):
        return attend_block(*pieces, lambdas, head_gain)
    grouped = tuple((a.reshape((N_EP, TOK_GRP) + a.shape[1:]) for a in (query, new_key, new_value, key_cache, value_cache, lengths)))
    attended = lax.map(one_group, grouped).reshape(rows, HEADS * VH)
    summed = ALPHA * tokens.astype(f32) + jnp.dot(attended, output_weight, preferred_element_type=f32)
    settled = norm_rows(summed, norm1_gain).astype(bf16)
    route_weight = jax.nn.softmax(route_logits, axis=-1)
    routes_grouped = routes.reshape(N_EP, TOK_GRP, TOPK)

    def dispatch(pieces):
        rows_block, routes_block = pieces
        chosen = choose_slots(routes_block, EXPERTS, CAP)
        placing = lax.optimization_barrier(jnp.sum(chosen.reshape(TOK_GRP, TOPK, -1).astype(f32), axis=1)).astype(bf16)
        sent = jnp.dot(placing.T, rows_block, preferred_element_type=f32)
        return sent.astype(bf16)
    sends = lax.map(dispatch, (settled.reshape(N_EP, TOK_GRP, D), routes_grouped))
    sends = jnp.moveaxis(sends.reshape(N_EP, EXPERTS, CAP, D), 1, 0)
    block = FF // N_TP

    def run_expert(pieces):
        rows_e, gate_e, up_e, down_e = pieces
        gate_h = jnp.einsum('scd,df->scf', rows_e.astype(f32), gate_e.astype(f32))
        up_h = jnp.einsum('scd,df->scf', rows_e.astype(f32), up_e.astype(f32))
        clipped = jnp.minimum(gate_h, LIMIT)
        linear = jnp.clip(up_h, -LIMIT, LIMIT)
        act = (clipped * jax.nn.sigmoid(SLOPE * clipped) * (linear + 1.0)).astype(bf16)
        total = jnp.zeros(rows_e.shape, f32)
        for index in range(N_TP):
            piece = jnp.einsum('scf,fd->scd', act[..., index * block:(index + 1) * block].astype(f32), down_e[index * block:(index + 1) * block].astype(f32))
            rounded = lax.optimization_barrier(piece.astype(bf16))
            total = total + rounded.astype(f32)
        return total.astype(bf16)
    answers = lax.map(run_expert, (sends, gate_weight, up_weight, down_weight))
    answers = jnp.moveaxis(answers, 1, 0).reshape(N_EP, EXPERTS * CAP, D)

    def combine(pieces):
        answers_block, routes_block = pieces
        chosen = choose_slots(routes_block, EXPERTS, CAP)
        picked = jnp.dot(chosen.astype(bf16), answers_block, preferred_element_type=f32)
        return picked.reshape(TOK_GRP, TOPK, D)
    picked = lax.map(combine, (answers, routes_grouped)).reshape(rows, TOPK, D)
    routed = lax.optimization_barrier(jnp.sum(picked * route_weight[:, :, None], axis=1))
    return norm_rows(ALPHA * settled.astype(f32) + routed, norm2_gain).astype(bf16)
```

```python
import functools
import math

import jax
import jax.numpy as jnp
from jax import lax
from jax.experimental import pallas as pl
from jax.experimental.pallas import tpu as pltpu
from jax.sharding import PartitionSpec as P

ALPHA = 1.4142135623730951
EPS = 1e-05
THETA = 500000.0
LIMIT = 7.0
SLOPE = 1.702
LANES = 128
MESH = pl.DeviceIdType.MESH
BF16 = jnp.bfloat16
F32 = jnp.float32


def repeat(count, step):
    if count <= 32:
        for i in range(count):
            step(i)
    else:
        lax.fori_loop(0, count, lambda i, _: (step(i), 0)[1], 0)


def column(values, rows):
    row = lax.broadcasted_iota(jnp.int32, (rows, LANES), 0)
    out = jnp.zeros((rows, LANES), F32)
    for r, value in enumerate(values):
        out = jnp.where(row == r, value, out)
    return out


def turns(positions, head_dim):
    half = head_dim // 2
    lane = lax.broadcasted_iota(jnp.int32, positions.shape, 1)
    index = lane % half
    freq = jnp.ones(positions.shape, F32)
    for bit in range(half.bit_length() - 1):
        factor = THETA ** (-(1 << bit) / half)
        freq = jnp.where((index // (1 << bit)) % 2 == 1, freq * factor, freq)
    angle = positions * freq
    sine = jnp.sin(angle)
    return jnp.cos(angle), jnp.where(lane % head_dim < half, -sine, sine)


def turn(values, cosine, sine, head_dim):
    half = head_dim // 2
    lane = lax.broadcasted_iota(jnp.int32, values.shape, 1)
    ahead = pltpu.roll(values, LANES - half, 1)
    behind = pltpu.roll(values, half, 1)
    other = jnp.where(lane % head_dim < half, ahead, behind)
    return values * cosine + other * sine


def kernel(
    n_ep, n_tp, head_dim,
    tokens_h, lengths_h, kc_h, vc_h, qw_h, kw_h, vw_h, lambdas_h, hg_h, ow_h, g1_h,
    routes_h, logits_h, gw_h, uw_h, dw_h, g2_h,
    out_ref,
    tok, lens, kc, vc, qw, kw, vw, lam, hg, ow, g1, routes, logits, gw, uw, dw, g2,
    tokf, qsend, qrecv, att, sm, blocks, wall, zs, zr, zm, rs, rr, st,
    in_sem, tok_s, tok_r, q_s, q_r, att_s, att_r, w_s, w_r,
    b_s, b_r, f_s, f_r, z_s, z_r, r_s, r_r, st_s, st_r,
):
    e = lax.axis_index("ep")
    t = lax.axis_index("tp")
    core = lax.rem(e, 2)
    chip = e // 2
    other = 1 - core
    sibling = chip * 2 + other
    n_dev = n_ep * n_tp
    nh = n_ep // 2
    n_same = nh * n_tp
    own, width = tokens_h.shape
    group = own * n_tp
    part = width // n_tp
    heads = lambdas_h.shape[0]
    heads_here = heads // n_tp
    topk = routes_h.shape[1]
    length = kc_h.shape[1]
    flat = e * n_tp + t

    barrier = pltpu.get_barrier_semaphore()

    def greet(i):
        peer = lax.rem(flat + i + 1, n_dev)
        pl.semaphore_signal(
            barrier, inc=1, device_id=(peer // n_tp, lax.rem(peer, n_tp)), device_id_type=MESH
        )

    repeat(n_dev - 1, greet)

    pairs = [
        (tokens_h, tok.at[t]), (lengths_h, lens), (routes_h, routes), (logits_h, logits),
        (kw_h, kw), (vw_h, vw), (qw_h, qw), (lambdas_h, lam), (hg_h, hg), (g1_h, g1), (g2_h, g2),
        (kc_h, kc), (vc_h, vc), (ow_h, ow), (gw_h.at[0], gw), (uw_h.at[0], uw), (dw_h.at[0], dw),
    ]
    loads = [pltpu.make_async_copy(a, b, in_sem.at[i]) for i, (a, b) in enumerate(pairs)]
    for load in loads:
        load.start()
    (l_tok, l_len, l_routes, l_logits, l_kw, l_vw, l_qw, l_lam, l_hg, l_g1, l_g2,
     l_kc, l_vc, l_ow, l_gw, l_uw, l_dw) = loads

    l_routes.wait()
    l_logits.wait()
    raw = logits[...]
    grown = jnp.exp(raw - jnp.max(raw, axis=1, keepdims=True))
    share = grown / jnp.sum(grown, axis=1, keepdims=True)
    named = routes[...]
    lanes = wall.shape[2]
    lane_w = lax.broadcasted_iota(jnp.int32, (group, lanes), 1)
    dense = jnp.zeros((group, lanes), F32)
    for k in range(topk):
        dense = jnp.where(named[:, k:k + 1] == lane_w, share[:, k:k + 1], dense)
    my_slot = core * nh + chip
    wall[my_slot] = dense

    l_len.wait()
    cos_g, sin_g = turns(column([lens[r].astype(F32) for r in range(group)], group), head_dim)
    own_lens = [lens[t * own + r] for r in range(own)]
    cos_o, sin_o = turns(column([v.astype(F32) for v in own_lens], own), head_dim)

    l_tok.wait()
    pl.semaphore_wait(barrier, n_dev - 1)

    def swap(ref, send, recv, src_of=None):
        copies = []
        for d in range(1, n_tp):
            to = lax.rem(t + d, n_tp)
            src = ref.at[t] if src_of is None else src_of.at[to]
            copies.append(pltpu.make_async_remote_copy(
                src_ref=src, dst_ref=ref.at[t], send_sem=send.at[d - 1], recv_sem=recv.at[d - 1],
                device_id=(e, to), device_id_type=MESH,
            ))
        for copy in copies:
            copy.start()
        return copies

    tok_copies = swap(tok, tok_s, tok_r)

    def send_w(i):
        to = lax.rem(e + i + 1, n_ep)
        pltpu.make_async_remote_copy(
            src_ref=wall.at[my_slot], dst_ref=wall.at[my_slot], send_sem=w_s, recv_sem=w_r,
            device_id=(to, t), device_id_type=MESH,
        ).start()

    repeat(n_ep - 1, send_w)

    mine = tok[t]
    l_kw.wait()
    new_key = jnp.dot(mine, kw[...], preferred_element_type=F32)
    new_key = turn(new_key, cos_o, sin_o, head_dim).astype(BF16).astype(F32)
    l_vw.wait()
    new_value = jnp.dot(mine, vw[...], preferred_element_type=F32).astype(BF16).astype(F32)

    l_qw.wait()
    for copy in tok_copies:
        copy.wait_recv()
    for s in range(n_tp):
        tokf[s * own:(s + 1) * own, :] = tok[s].astype(F32)
    query = jnp.dot(tokf[...].astype(BF16), qw[...], preferred_element_type=F32)
    for h in range(heads_here):
        cut = slice(h * LANES, (h + 1) * LANES)
        turned = turn(query[:, cut], cos_g, sin_g, head_dim)
        for s in range(n_tp):
            qsend[s, :, cut] = turned[s * own:(s + 1) * own, :].astype(BF16)
    q_copies = swap(qrecv, q_s, q_r, qsend)
    qrecv[t] = qsend[t]

    l_lam.wait()
    l_hg.wait()
    l_kc.wait()
    l_vc.wait()
    for copy in q_copies:
        copy.wait_recv()

    scale = head_dim ** (-0.5)
    rows2 = 2 * heads
    row = lax.broadcasted_iota(jnp.int32, (rows2, LANES), 0)
    lane = lax.broadcasted_iota(jnp.int32, (rows2, LANES), 1)
    my_map = (row // heads) == (lane // head_dim)
    position = lax.broadcasted_iota(jnp.int32, (rows2, length), 1)
    mixing = column([lam[h] for h in range(heads)], heads)[:, :1]
    queries = [qrecv[s].astype(F32) for s in range(n_tp)]
    outs = []
    for b in range(own):
        qm = jnp.zeros((rows2, LANES), F32)
        for h in range(heads):
            at = (h % heads_here) * LANES
            piece = queries[h // heads_here][b:b + 1, at:at + LANES]
            qm = jnp.where(row % heads == h, piece, qm)
        qm = jnp.where(my_map, qm, 0.0)
        past = lax.dot_general(
            qm.astype(BF16), kc[b], (((1,), (1,)), ((), ())), preferred_element_type=F32
        ) * scale
        past = jnp.where(position < own_lens[b], past, -jnp.inf)
        selfs = jnp.sum(qm * new_key[b:b + 1, :], axis=1, keepdims=True) * scale
        top = jnp.maximum(jnp.max(past, axis=1, keepdims=True), selfs)
        past_exp = jnp.exp(past - top)
        self_exp = jnp.exp(selfs - top)
        total = jnp.sum(past_exp, axis=1, keepdims=True) + self_exp
        past_prob = past_exp / total
        self_prob = self_exp / total
        weight = (past_prob[:heads] - mixing * past_prob[heads:]).astype(BF16)
        self_weight = (self_prob[:heads] - mixing * self_prob[heads:]).astype(BF16).astype(F32)
        head_out = jnp.dot(weight, vc[b], preferred_element_type=F32)
        head_out = head_out + self_weight * new_value[b:b + 1, :]
        square = jnp.mean(head_out * head_out, axis=1, keepdims=True)
        outs.append(head_out * lax.rsqrt(square + EPS) * hg[...])
    row_o = lax.broadcasted_iota(jnp.int32, (own, LANES), 0)
    for h in range(heads):
        piece = jnp.zeros((own, LANES), F32)
        for b in range(own):
            piece = jnp.where(row_o == b, outs[b][h:h + 1, :], piece)
        att[t, :, h * LANES:(h + 1) * LANES] = piece.astype(BF16)
    att_copies = swap(att, att_s, att_r)

    l_ow.wait()
    l_g1.wait()
    l_g2.wait()
    cols = pl.ds(pl.multiple_of(t * part, LANES), part)
    for copy in att_copies:
        copy.wait_recv()
    for s in range(n_tp):
        sm[s * own:(s + 1) * own, :] = att[s].astype(F32)
    mix = jnp.dot(sm[...].astype(BF16), ow[...], preferred_element_type=F32)
    summed = ALPHA * tokf[:, cols] + mix
    blocks[core, t, chip] = summed.astype(BF16)

    rank = chip * n_tp + t

    def send_block(i):
        to = lax.rem(rank + i + 1, n_same)
        pltpu.make_async_remote_copy(
            src_ref=blocks.at[core, t, chip], dst_ref=blocks.at[core, t, chip],
            send_sem=b_s, recv_sem=b_r.at[i],
            device_id=(to // n_tp * 2 + core, lax.rem(to, n_tp)), device_id_type=MESH,
        ).start()

    repeat(n_same - 1, send_block)

    def forward(src):
        at = blocks.at[core, lax.rem(src, n_tp), src // n_tp]
        pltpu.make_async_remote_copy(
            src_ref=at, dst_ref=at, send_sem=f_s, recv_sem=f_r,
            device_id=(sibling, t), device_id_type=MESH,
        ).start()

    forward(rank)

    def take_block(i):
        src = lax.rem(rank - (i + 1) + n_same, n_same)
        at = blocks.at[core, lax.rem(src, n_tp), src // n_tp]
        pltpu.make_async_remote_copy(
            src_ref=at, dst_ref=at, send_sem=b_s, recv_sem=b_r.at[i],
            device_id=(sibling, t), device_id_type=MESH,
        ).wait_recv()
        forward(src)

    repeat(n_same - 1, take_block)

    def await_bytes(ref, sem):
        pltpu.make_async_copy(ref, ref, sem).wait()

    await_bytes(wall.at[pl.ds(0, n_ep - 1)], w_r)
    l_gw.wait()
    l_uw.wait()
    l_dw.wait()

    count = max(1, min(nh, 128 // group))
    rows = count * group

    def settle(pieces, gains):
        mean = sum(jnp.sum(x, axis=-1, keepdims=True) for x in pieces) / width
        pieces = [x - mean for x in pieces]
        spread = sum(jnp.sum(x * x, axis=-1, keepdims=True) for x in pieces) / width
        inverse = lax.rsqrt(spread + EPS)
        return [x * inverse * g for x, g in zip(pieces, gains)]

    gains = [g1[:, s * part:(s + 1) * part] for s in range(n_tp)]

    def expert(parity, store):
        def step(c):
            first = c * count
            pieces = [
                blocks[parity, s, pl.ds(first, count)].astype(F32).reshape(rows, part)
                for s in range(n_tp)
            ]
            x = jnp.concatenate([v.astype(BF16) for v in settle(pieces, gains)], axis=1)
            gate = jnp.dot(x, gw[...], preferred_element_type=F32)
            up = jnp.dot(x, uw[...], preferred_element_type=F32)
            clipped = jnp.minimum(gate, LIMIT)
            linear = jnp.clip(up, -LIMIT, LIMIT)
            act = (clipped * jax.nn.sigmoid(SLOPE * clipped) * (linear + 1.0)).astype(BF16)
            dense = wall[pl.ds(parity * nh + first, count)].reshape(rows, lanes)
            lane_e = lax.broadcasted_iota(jnp.int32, dense.shape, 1)
            share = jnp.sum(jnp.where(lane_e == e, dense, 0.0), axis=1, keepdims=True)
            terms = jnp.dot(act, dw[...], preferred_element_type=F32) * share
            for s in range(n_tp):
                store(s, first, terms[:, s * part:(s + 1) * part].reshape(count, group, part))

        repeat(nh // count, step)

    def store_sibling(s, first, value):
        zs[s, pl.ds(first, count)] = value.astype(BF16)

    def store_mine(s, first, value):
        zm[s, pl.ds(first, count)] = value

    expert(core, store_sibling)
    z_copy = pltpu.make_async_remote_copy(
        src_ref=zs, dst_ref=zr, send_sem=z_s, recv_sem=z_r,
        device_id=(sibling, t), device_id_type=MESH,
    )
    z_copy.start()
    await_bytes(blocks.at[other], f_r)
    expert(other, store_mine)
    z_copy.wait_recv()

    def add_chunk(c):
        at = pl.ds(c * count, count)
        for s in range(n_tp):
            rs[s, at] = (zm[s, at] + zr[s, at].astype(F32)).astype(BF16)

    repeat(nh // count, add_chunk)

    def send_result(i):
        to = lax.rem(rank + i, n_same)
        to_chip = to // n_tp
        to_tp = lax.rem(to, n_tp)
        pltpu.make_async_remote_copy(
            src_ref=rs.at[to_tp, to_chip], dst_ref=rr.at[t, chip], send_sem=r_s, recv_sem=r_r,
            device_id=(to_chip * 2 + other, to_tp), device_id_type=MESH,
        ).start()

    repeat(n_same, send_result)

    pieces = [blocks[core, s, chip].astype(F32) for s in range(n_tp)]
    mean = sum(jnp.sum(x, axis=1, keepdims=True) for x in pieces) / width
    spread = sum(jnp.sum((x - mean) * (x - mean), axis=1, keepdims=True) for x in pieces) / width
    here = blocks[core, t, chip].astype(F32)
    settled = ((here - mean) * lax.rsqrt(spread + EPS) * g1[:, cols]).astype(BF16).astype(F32)

    await_bytes(rr, r_r)
    final = ALPHA * settled
    if n_same <= 32:
        for s in range(n_tp):
            for c in range(nh):
                final = final + rr[s, c].astype(F32)
    else:
        def add(i, total):
            return total + rr[lax.rem(i, n_tp), i // n_tp].astype(F32)

        final = lax.fori_loop(0, n_same, add, final)
    lane_s = lax.broadcasted_iota(jnp.int32, (group, LANES), 1)
    sums = jnp.sum(final, axis=1, keepdims=True)
    squares = jnp.sum(final * final, axis=1, keepdims=True)
    st[t] = jnp.where(lane_s == 0, sums, squares)
    st_copies = swap(st, st_s, st_r)
    for copy in st_copies:
        copy.wait_recv()
    stats = sum(st[s] for s in range(n_tp)) / width
    mean = stats[:, 0:1]
    spread = stats[:, 1:2] - mean * mean
    out_ref[...] = ((final - mean) * lax.rsqrt(spread + EPS) * g2[:, cols]).astype(BF16)

    for copy in tok_copies + q_copies + att_copies + st_copies + [z_copy]:
        copy.wait_send()
    await_bytes(wall.at[pl.ds(0, n_ep - 1)], w_s)
    await_bytes(rr, r_s)
    await_bytes(blocks.at[core], f_s)
    if n_tp > 1:
        await_bytes(blocks.at[core, pl.ds(0, n_tp - 1)], b_s)
    await_bytes(blocks.at[core, 0, pl.ds(0, nh - 1)], b_s)


def body(mesh_shape, *args):
    (tokens, lengths, key_cache, value_cache, query_weight, key_weight, value_weight, lambdas,
     head_gain, output_weight, norm1_gain, routes, route_logits, gate_weight, up_weight,
     down_weight, norm2_gain) = args
    n_ep, n_tp = mesh_shape
    own, width = tokens.shape
    group = own * n_tp
    part = width // n_tp
    nh = n_ep // 2
    n_same = nh * n_tp
    heads = lambdas.shape[0]
    value_dim = value_weight.shape[1]
    head_dim = key_weight.shape[1] // 2
    lanes = -(-n_ep // LANES) * LANES
    operands = (
        tokens, lengths, key_cache, value_cache, query_weight, key_weight, value_weight, lambdas,
        head_gain.reshape(1, -1), output_weight, norm1_gain.reshape(1, -1), routes, route_logits,
        gate_weight, up_weight, down_weight, norm2_gain.reshape(1, -1),
    )
    v = pltpu.VMEM
    dma = pltpu.SemaphoreType.DMA
    partners = max(1, n_tp - 1)
    scratch = [
        v((n_tp, own, width), BF16), pltpu.SMEM(lengths.shape, jnp.int32),
        v(key_cache.shape, BF16), v(value_cache.shape, BF16), v(query_weight.shape, BF16),
        v(key_weight.shape, BF16), v(value_weight.shape, BF16), pltpu.SMEM(lambdas.shape, F32),
        v((1, value_dim), F32), v(output_weight.shape, BF16), v((1, width), F32),
        v(routes.shape, jnp.int32), v(route_logits.shape, F32), v(gate_weight.shape[1:], BF16),
        v(up_weight.shape[1:], BF16), v(down_weight.shape[1:], BF16), v((1, width), F32),
        v((group, width), F32),
        v((n_tp, own, query_weight.shape[1]), BF16), v((n_tp, own, query_weight.shape[1]), BF16),
        v((n_tp, own, heads * value_dim), BF16), v((group, heads * value_dim), F32),
        v((2, n_tp, nh, group, part), BF16), v((n_ep, group, lanes), F32),
        v((n_tp, nh, group, part), BF16), v((n_tp, nh, group, part), BF16),
        v((n_tp, nh, group, part), F32), v((n_tp, nh, group, part), BF16),
        v((n_tp, nh, group, part), BF16), v((n_tp, group, LANES), F32),
        dma((len(operands),)), dma((partners,)), dma((partners,)), dma((partners,)),
        dma((partners,)), dma((partners,)), dma((partners,)), dma, dma,
        dma, dma((n_same - 1,)), dma, dma, dma, dma, dma, dma, dma((partners,)), dma((partners,)),
    ]
    return pl.pallas_call(
        functools.partial(kernel, n_ep, n_tp, head_dim),
        out_shape=jax.ShapeDtypeStruct((group, part), BF16),
        in_specs=[pl.BlockSpec(memory_space=pl.ANY)] * len(operands),
        out_specs=pl.BlockSpec(memory_space=pltpu.VMEM),
        scratch_shapes=scratch,
        compiler_params=pltpu.CompilerParams(
            collective_id=0, has_side_effects=True, vmem_limit_bytes=60 * 1024 * 1024
        ),
    )(*operands)


def solution(mesh):
    in_specs = (
        P(("ep", "tp"), None),
        P("ep"),
        P(("ep", "tp"), None, None),
        P(("ep", "tp"), None, None),
        P(None, "tp"),
        P(),
        P(),
        P(),
        P(),
        P(None, "tp"),
        P(),
        P("ep", None),
        P("ep", None),
        P("ep", None, "tp"),
        P("ep", None, "tp"),
        P("ep", "tp", None),
        P(),
    )
    out_specs = P("ep", "tp")
    shape = (mesh.shape["ep"], mesh.shape["tp"])
    return jax.shard_map(
        functools.partial(body, shape), mesh=mesh, in_specs=in_specs, out_specs=out_specs,
        check_vma=False,
    )
```

```python
import functools
import math

import jax
import jax.numpy as jnp
from jax import lax
from jax.experimental import pallas as pl
from jax.experimental.pallas import tpu as pltpu
from jax.sharding import PartitionSpec as P

ALPHA = 1.4142135623730951
EPS = 1e-05
THETA = 500000.0
LIMIT = 7.0
SLOPE = 1.702
LANES = 128
MESH = pl.DeviceIdType.MESH
BF16 = jnp.bfloat16
F32 = jnp.float32


def repeat(count, step):
    if count <= 32:
        for i in range(count):
            step(i)
    else:
        lax.fori_loop(0, count, lambda i, _: (step(i), 0)[1], 0)


def column(values, rows):
    row = lax.broadcasted_iota(jnp.int32, (rows, LANES), 0)
    out = jnp.zeros((rows, LANES), F32)
    for r, value in enumerate(values):
        out = jnp.where(row == r, value, out)
    return out


def turns(positions, head_dim):
    half = head_dim // 2
    lane = lax.broadcasted_iota(jnp.int32, positions.shape, 1)
    index = lane % half
    freq = jnp.ones(positions.shape, F32)
    for bit in range(half.bit_length() - 1):
        factor = THETA ** (-(1 << bit) / half)
        freq = jnp.where((index // (1 << bit)) % 2 == 1, freq * factor, freq)
    angle = positions * freq
    sine = jnp.sin(angle)
    return jnp.cos(angle), jnp.where(lane % head_dim < half, -sine, sine)


def turn(values, cosine, sine, head_dim):
    half = head_dim // 2
    lane = lax.broadcasted_iota(jnp.int32, values.shape, 1)
    ahead = pltpu.roll(values, LANES - half, 1)
    behind = pltpu.roll(values, half, 1)
    other = jnp.where(lane % head_dim < half, ahead, behind)
    return values * cosine + other * sine


def kernel(
    n_ep, n_tp, head_dim,
    tokens_h, lengths_h, kc_h, vc_h, qw_h, kw_h, vw_h, lambdas_h, hg_h, ow_h, g1_h,
    routes_h, logits_h, gw_h, uw_h, dw_h, g2_h,
    out_ref,
    tok, lens, kc, vc, qw, kw, vw, lam, hg, ow, g1, routes, logits, gw, uw, dw, g2,
    tokf, qsend, qrecv, att, sm, blocks, wall, zs, zr, zm, rs, rr, st,
    in_sem, tok_s, tok_r, q_s, q_r, att_s, att_r, w_s, w_r,
    b_s, b_r, f_s, f_r, z_s, z_r, r_s, r_r, st_s, st_r, round_s,
):
    e = lax.axis_index("ep")
    t = lax.axis_index("tp")
    core = lax.rem(e, 2)
    chip = e // 2
    other = 1 - core
    sibling = chip * 2 + other
    n_dev = n_ep * n_tp
    nh = n_ep // 2
    n_same = nh * n_tp
    own, width = tokens_h.shape
    group = own * n_tp
    part = width // n_tp
    heads = lambdas_h.shape[0]
    heads_here = heads // n_tp
    topk = routes_h.shape[1]
    length = kc_h.shape[1]
    flat = e * n_tp + t

    barrier = pltpu.get_barrier_semaphore()
    bits = (n_dev - 1).bit_length()

    def across(k):
        step = 1 << k
        peer = flat + step * (1 - 2 * lax.rem(flat // step, 2))
        return (peer // n_tp, lax.rem(peer, n_tp))

    for k in range(bits):
        pl.semaphore_signal(barrier, inc=1, device_id=across(k), device_id_type=MESH)

    def spread(k):
        pl.semaphore_signal(round_s.at[k], inc=1, device_id=across(k), device_id_type=MESH)
        pl.semaphore_wait(round_s.at[k], 1)

    pairs = [
        (tokens_h, tok.at[t]), (lengths_h, lens), (routes_h, routes), (logits_h, logits),
        (kw_h, kw), (vw_h, vw), (qw_h, qw), (lambdas_h, lam), (hg_h, hg), (g1_h, g1), (g2_h, g2),
        (kc_h, kc), (vc_h, vc), (ow_h, ow), (gw_h.at[0], gw), (uw_h.at[0], uw), (dw_h.at[0], dw),
    ]
    loads = [pltpu.make_async_copy(a, b, in_sem.at[i]) for i, (a, b) in enumerate(pairs)]
    for load in loads:
        load.start()
    (l_tok, l_len, l_routes, l_logits, l_kw, l_vw, l_qw, l_lam, l_hg, l_g1, l_g2,
     l_kc, l_vc, l_ow, l_gw, l_uw, l_dw) = loads

    l_routes.wait()
    l_logits.wait()
    raw = logits[...]
    grown = jnp.exp(raw - jnp.max(raw, axis=1, keepdims=True))
    share = grown / jnp.sum(grown, axis=1, keepdims=True)
    named = routes[...]
    lanes = wall.shape[2]
    lane_w = lax.broadcasted_iota(jnp.int32, (group, lanes), 1)
    dense = jnp.zeros((group, lanes), F32)
    for k in range(topk):
        dense = jnp.where(named[:, k:k + 1] == lane_w, share[:, k:k + 1], dense)
    my_slot = core * nh + chip
    wall[my_slot] = dense

    l_len.wait()
    cos_g, sin_g = turns(column([lens[r].astype(F32) for r in range(group)], group), head_dim)
    own_lens = [lens[t * own + r] for r in range(own)]
    cos_o, sin_o = turns(column([v.astype(F32) for v in own_lens], own), head_dim)

    l_tok.wait()
    pl.semaphore_wait(barrier, bits)

    def swap(ref, send, recv, src_of=None):
        copies = []
        for d in range(1, n_tp):
            to = lax.rem(t + d, n_tp)
            src = ref.at[t] if src_of is None else src_of.at[to]
            copies.append(pltpu.make_async_remote_copy(
                src_ref=src, dst_ref=ref.at[t], send_sem=send.at[d - 1], recv_sem=recv.at[d - 1],
                device_id=(e, to), device_id_type=MESH,
            ))
        for copy in copies:
            copy.start()
        return copies

    tok_copies = swap(tok, tok_s, tok_r)

    def send_w(i):
        to = lax.rem(e + i + 1, n_ep)
        pltpu.make_async_remote_copy(
            src_ref=wall.at[my_slot], dst_ref=wall.at[my_slot], send_sem=w_s, recv_sem=w_r,
            device_id=(to, t), device_id_type=MESH,
        ).start()


    mine = tok[t]
    l_kw.wait()
    new_key = jnp.dot(mine, kw[...], preferred_element_type=F32)
    new_key = turn(new_key, cos_o, sin_o, head_dim).astype(BF16).astype(F32)
    l_vw.wait()
    new_value = jnp.dot(mine, vw[...], preferred_element_type=F32).astype(BF16).astype(F32)

    l_qw.wait()
    for k in range(1, min(4, bits)):
        spread(k)
    for copy in tok_copies:
        copy.wait_recv()
    for s in range(n_tp):
        tokf[s * own:(s + 1) * own, :] = tok[s].astype(F32)
    query = jnp.dot(tokf[...].astype(BF16), qw[...], preferred_element_type=F32)
    for h in range(heads_here):
        cut = slice(h * LANES, (h + 1) * LANES)
        turned = turn(query[:, cut], cos_g, sin_g, head_dim)
        for s in range(n_tp):
            qsend[s, :, cut] = turned[s * own:(s + 1) * own, :].astype(BF16)
    q_copies = swap(qrecv, q_s, q_r, qsend)
    qrecv[t] = qsend[t]
    for k in range(4, bits):
        spread(k)
    repeat(n_ep - 1, send_w)

    l_lam.wait()
    l_hg.wait()
    l_kc.wait()
    l_vc.wait()
    for copy in q_copies:
        copy.wait_recv()

    scale = head_dim ** (-0.5)
    rows2 = 2 * heads
    row = lax.broadcasted_iota(jnp.int32, (rows2, LANES), 0)
    lane = lax.broadcasted_iota(jnp.int32, (rows2, LANES), 1)
    my_map = (row // heads) == (lane // head_dim)
    position = lax.broadcasted_iota(jnp.int32, (rows2, length), 1)
    mixing = column([lam[h] for h in range(heads)], heads)[:, :1]
    queries = [qrecv[s].astype(F32) for s in range(n_tp)]
    outs = []
    for b in range(own):
        qm = jnp.zeros((rows2, LANES), F32)
        for h in range(heads):
            at = (h % heads_here) * LANES
            piece = queries[h // heads_here][b:b + 1, at:at + LANES]
            qm = jnp.where(row % heads == h, piece, qm)
        qm = jnp.where(my_map, qm, 0.0)
        past = lax.dot_general(
            qm.astype(BF16), kc[b], (((1,), (1,)), ((), ())), preferred_element_type=F32
        ) * scale
        past = jnp.where(position < own_lens[b], past, -jnp.inf)
        selfs = jnp.sum(qm * new_key[b:b + 1, :], axis=1, keepdims=True) * scale
        top = jnp.maximum(jnp.max(past, axis=1, keepdims=True), selfs)
        past_exp = jnp.exp(past - top)
        self_exp = jnp.exp(selfs - top)
        total = jnp.sum(past_exp, axis=1, keepdims=True) + self_exp
        past_prob = past_exp / total
        self_prob = self_exp / total
        weight = (past_prob[:heads] - mixing * past_prob[heads:]).astype(BF16)
        self_weight = (self_prob[:heads] - mixing * self_prob[heads:]).astype(BF16).astype(F32)
        head_out = jnp.dot(weight, vc[b], preferred_element_type=F32)
        head_out = head_out + self_weight * new_value[b:b + 1, :]
        square = jnp.mean(head_out * head_out, axis=1, keepdims=True)
        outs.append(head_out * lax.rsqrt(square + EPS) * hg[...])
    row_o = lax.broadcasted_iota(jnp.int32, (own, LANES), 0)
    for h in range(heads):
        piece = jnp.zeros((own, LANES), F32)
        for b in range(own):
            piece = jnp.where(row_o == b, outs[b][h:h + 1, :], piece)
        att[t, :, h * LANES:(h + 1) * LANES] = piece.astype(BF16)
    att_copies = swap(att, att_s, att_r)

    l_ow.wait()
    l_g1.wait()
    l_g2.wait()
    cols = pl.ds(pl.multiple_of(t * part, LANES), part)
    for copy in att_copies:
        copy.wait_recv()
    for s in range(n_tp):
        sm[s * own:(s + 1) * own, :] = att[s].astype(F32)
    mix = jnp.dot(sm[...].astype(BF16), ow[...], preferred_element_type=F32)
    summed = ALPHA * tokf[:, cols] + mix
    blocks[core, t, chip] = summed.astype(BF16)

    rank = chip * n_tp + t
    low = rank < n_same // 2

    def send_block(i):
        v = jnp.where(low, n_same - 2 - i, i)
        to = v + (v >= rank).astype(jnp.int32)
        pltpu.make_async_remote_copy(
            src_ref=blocks.at[core, t, chip], dst_ref=blocks.at[core, t, chip],
            send_sem=b_s, recv_sem=b_r.at[rank],
            device_id=(to // n_tp * 2 + core, lax.rem(to, n_tp)), device_id_type=MESH,
        ).start()

    repeat(n_same - 1, send_block)

    def forward(src):
        at = blocks.at[core, lax.rem(src, n_tp), src // n_tp]
        pltpu.make_async_remote_copy(
            src_ref=at, dst_ref=at, send_sem=f_s, recv_sem=f_r,
            device_id=(sibling, t), device_id_type=MESH,
        ).start()

    forward(rank)

    def take_block(i):
        src = lax.rem(rank - (i + 1) + n_same, n_same)
        at = blocks.at[core, lax.rem(src, n_tp), src // n_tp]
        pltpu.make_async_remote_copy(
            src_ref=at, dst_ref=at, send_sem=b_s, recv_sem=b_r.at[src],
            device_id=(sibling, t), device_id_type=MESH,
        ).wait_recv()
        forward(src)

    repeat(n_same - 1, take_block)

    def await_bytes(ref, sem):
        pltpu.make_async_copy(ref, ref, sem).wait()

    await_bytes(wall.at[pl.ds(0, n_ep - 1)], w_r)
    l_gw.wait()
    l_uw.wait()
    l_dw.wait()

    count = max(1, min(nh, 128 // group))
    rows = count * group

    def settle(pieces, gains):
        mean = sum(jnp.sum(x, axis=-1, keepdims=True) for x in pieces) / width
        pieces = [x - mean for x in pieces]
        spread = sum(jnp.sum(x * x, axis=-1, keepdims=True) for x in pieces) / width
        inverse = lax.rsqrt(spread + EPS)
        return [x * inverse * g for x, g in zip(pieces, gains)]

    gains = [g1[:, s * part:(s + 1) * part] for s in range(n_tp)]

    def expert(parity, store):
        def step(c):
            first = c * count
            pieces = [
                blocks[parity, s, pl.ds(first, count)].astype(F32).reshape(rows, part)
                for s in range(n_tp)
            ]
            x = jnp.concatenate([v.astype(BF16) for v in settle(pieces, gains)], axis=1)
            gate = jnp.dot(x, gw[...], preferred_element_type=F32)
            up = jnp.dot(x, uw[...], preferred_element_type=F32)
            clipped = jnp.minimum(gate, LIMIT)
            linear = jnp.clip(up, -LIMIT, LIMIT)
            act = (clipped * jax.nn.sigmoid(SLOPE * clipped) * (linear + 1.0)).astype(BF16)
            dense = wall[pl.ds(parity * nh + first, count)].reshape(rows, lanes)
            lane_e = lax.broadcasted_iota(jnp.int32, dense.shape, 1)
            share = jnp.sum(jnp.where(lane_e == e, dense, 0.0), axis=1, keepdims=True)
            terms = jnp.dot(act, dw[...], preferred_element_type=F32) * share
            for s in range(n_tp):
                store(s, first, terms[:, s * part:(s + 1) * part].reshape(count, group, part))

        repeat(nh // count, step)

    def store_sibling(s, first, value):
        zs[s, pl.ds(first, count)] = value.astype(BF16)

    def store_mine(s, first, value):
        zm[s, pl.ds(first, count)] = value

    expert(core, store_sibling)
    z_copy = pltpu.make_async_remote_copy(
        src_ref=zs, dst_ref=zr, send_sem=z_s, recv_sem=z_r,
        device_id=(sibling, t), device_id_type=MESH,
    )
    z_copy.start()
    await_bytes(blocks.at[other], f_r)
    expert(other, store_mine)
    z_copy.wait_recv()

    def add_chunk(c):
        at = pl.ds(c * count, count)
        for s in range(n_tp):
            rs[s, at] = (zm[s, at] + zr[s, at].astype(F32)).astype(BF16)

    repeat(nh // count, add_chunk)

    def send_result(i):
        to = jnp.where(low, n_same - 1 - i, i)
        to_chip = to // n_tp
        to_tp = lax.rem(to, n_tp)
        pltpu.make_async_remote_copy(
            src_ref=rs.at[to_tp, to_chip], dst_ref=rr.at[t, chip], send_sem=r_s, recv_sem=r_r,
            device_id=(to_chip * 2 + other, to_tp), device_id_type=MESH,
        ).start()

    repeat(n_same, send_result)

    pieces = [blocks[core, s, chip].astype(F32) for s in range(n_tp)]
    mean = sum(jnp.sum(x, axis=1, keepdims=True) for x in pieces) / width
    spread = sum(jnp.sum((x - mean) * (x - mean), axis=1, keepdims=True) for x in pieces) / width
    here = blocks[core, t, chip].astype(F32)
    settled = ((here - mean) * lax.rsqrt(spread + EPS) * g1[:, cols]).astype(BF16).astype(F32)

    await_bytes(rr, r_r)
    final = ALPHA * settled
    if n_same <= 32:
        for s in range(n_tp):
            for c in range(nh):
                final = final + rr[s, c].astype(F32)
    else:
        def add(i, total):
            return total + rr[lax.rem(i, n_tp), i // n_tp].astype(F32)

        final = lax.fori_loop(0, n_same, add, final)
    lane_s = lax.broadcasted_iota(jnp.int32, (group, LANES), 1)
    sums = jnp.sum(final, axis=1, keepdims=True)
    squares = jnp.sum(final * final, axis=1, keepdims=True)
    st[t] = jnp.where(lane_s == 0, sums, squares)
    st_copies = swap(st, st_s, st_r)
    for copy in st_copies:
        copy.wait_recv()
    stats = sum(st[s] for s in range(n_tp)) / width
    mean = stats[:, 0:1]
    spread = stats[:, 1:2] - mean * mean
    out_ref[...] = ((final - mean) * lax.rsqrt(spread + EPS) * g2[:, cols]).astype(BF16)

    for copy in tok_copies + q_copies + att_copies + st_copies + [z_copy]:
        copy.wait_send()
    await_bytes(wall.at[pl.ds(0, n_ep - 1)], w_s)
    await_bytes(rr, r_s)
    await_bytes(blocks.at[core], f_s)
    if n_tp > 1:
        await_bytes(blocks.at[core, pl.ds(0, n_tp - 1)], b_s)
    await_bytes(blocks.at[core, 0, pl.ds(0, nh - 1)], b_s)


def body(mesh_shape, *args):
    (tokens, lengths, key_cache, value_cache, query_weight, key_weight, value_weight, lambdas,
     head_gain, output_weight, norm1_gain, routes, route_logits, gate_weight, up_weight,
     down_weight, norm2_gain) = args
    n_ep, n_tp = mesh_shape
    own, width = tokens.shape
    group = own * n_tp
    part = width // n_tp
    nh = n_ep // 2
    n_same = nh * n_tp
    heads = lambdas.shape[0]
    value_dim = value_weight.shape[1]
    head_dim = key_weight.shape[1] // 2
    lanes = -(-n_ep // LANES) * LANES
    operands = (
        tokens, lengths, key_cache, value_cache, query_weight, key_weight, value_weight, lambdas,
        head_gain.reshape(1, -1), output_weight, norm1_gain.reshape(1, -1), routes, route_logits,
        gate_weight, up_weight, down_weight, norm2_gain.reshape(1, -1),
    )
    v = pltpu.VMEM
    dma = pltpu.SemaphoreType.DMA
    partners = max(1, n_tp - 1)
    scratch = [
        v((n_tp, own, width), BF16), pltpu.SMEM(lengths.shape, jnp.int32),
        v(key_cache.shape, BF16), v(value_cache.shape, BF16), v(query_weight.shape, BF16),
        v(key_weight.shape, BF16), v(value_weight.shape, BF16), pltpu.SMEM(lambdas.shape, F32),
        v((1, value_dim), F32), v(output_weight.shape, BF16), v((1, width), F32),
        v(routes.shape, jnp.int32), v(route_logits.shape, F32), v(gate_weight.shape[1:], BF16),
        v(up_weight.shape[1:], BF16), v(down_weight.shape[1:], BF16), v((1, width), F32),
        v((group, width), F32),
        v((n_tp, own, query_weight.shape[1]), BF16), v((n_tp, own, query_weight.shape[1]), BF16),
        v((n_tp, own, heads * value_dim), BF16), v((group, heads * value_dim), F32),
        v((2, n_tp, nh, group, part), BF16), v((n_ep, group, lanes), F32),
        v((n_tp, nh, group, part), BF16), v((n_tp, nh, group, part), BF16),
        v((n_tp, nh, group, part), F32), v((n_tp, nh, group, part), BF16),
        v((n_tp, nh, group, part), BF16), v((n_tp, group, LANES), F32),
        dma((len(operands),)), dma((partners,)), dma((partners,)), dma((partners,)),
        dma((partners,)), dma((partners,)), dma((partners,)), dma, dma,
        dma, dma((n_same,)), dma, dma, dma, dma, dma, dma, dma((partners,)), dma((partners,)),
        pltpu.SemaphoreType.REGULAR(((n_ep * n_tp).bit_length(),)),
    ]
    return pl.pallas_call(
        functools.partial(kernel, n_ep, n_tp, head_dim),
        out_shape=pltpu.VMEM((group, part), BF16),
        in_specs=[pl.BlockSpec(memory_space=pl.ANY)] * len(operands),
        out_specs=pl.BlockSpec(memory_space=pltpu.VMEM),
        scratch_shapes=scratch,
        compiler_params=pltpu.CompilerParams(
            collective_id=0, has_side_effects=True, vmem_limit_bytes=60 * 1024 * 1024
        ),
    )(*operands)


def solution(mesh):
    in_specs = (
        P(("ep", "tp"), None),
        P("ep"),
        P(("ep", "tp"), None, None),
        P(("ep", "tp"), None, None),
        P(None, "tp"),
        P(),
        P(),
        P(),
        P(),
        P(None, "tp"),
        P(),
        P("ep", None),
        P("ep", None),
        P("ep", None, "tp"),
        P("ep", None, "tp"),
        P("ep", "tp", None),
        P(),
    )
    out_specs = P("ep", "tp")
    shape = (mesh.shape["ep"], mesh.shape["tp"])
    return jax.shard_map(
        functools.partial(body, shape), mesh=mesh, in_specs=in_specs, out_specs=out_specs,
        check_vma=False,
    )
```

```python
import functools
import math

import jax
import jax.numpy as jnp
from jax import lax
from jax.experimental import pallas as pl
from jax.experimental.pallas import tpu as pltpu
from jax.sharding import PartitionSpec as P

ALPHA = 1.4142135623730951
EPS = 1e-05
THETA = 500000.0
LIMIT = 7.0
SLOPE = 1.702
LANES = 128
MESH = pl.DeviceIdType.MESH
BF16 = jnp.bfloat16
F32 = jnp.float32


def repeat(count, step):
    if count <= 32:
        for i in range(count):
            step(i)
    else:
        lax.fori_loop(0, count, lambda i, _: (step(i), 0)[1], 0)


def column(values, rows):
    row = lax.broadcasted_iota(jnp.int32, (rows, LANES), 0)
    out = jnp.zeros((rows, LANES), F32)
    for r, value in enumerate(values):
        out = jnp.where(row == r, value, out)
    return out


def turns(positions, head_dim):
    half = head_dim // 2
    lane = lax.broadcasted_iota(jnp.int32, positions.shape, 1)
    index = lane % half
    freq = jnp.ones(positions.shape, F32)
    for bit in range(half.bit_length() - 1):
        factor = THETA ** (-(1 << bit) / half)
        freq = jnp.where((index // (1 << bit)) % 2 == 1, freq * factor, freq)
    angle = positions * freq
    sine = jnp.sin(angle)
    return jnp.cos(angle), jnp.where(lane % head_dim < half, -sine, sine)


def turn(values, cosine, sine, head_dim):
    half = head_dim // 2
    lane = lax.broadcasted_iota(jnp.int32, values.shape, 1)
    ahead = pltpu.roll(values, LANES - half, 1)
    behind = pltpu.roll(values, half, 1)
    other = jnp.where(lane % head_dim < half, ahead, behind)
    return values * cosine + other * sine


def kernel(
    n_ep, n_tp, head_dim,
    tokens_h, lengths_h, kc_h, vc_h, qw_h, kw_h, vw_h, lambdas_h, hg_h, ow_h, g1_h,
    routes_h, logits_h, gw_h, uw_h, dw_h, g2_h,
    out_ref,
    tok, lens, kc, vc, qw, kw, vw, lam, hg, ow, g1, routes, logits, gw, uw, dw, g2,
    tokf, qsend, qrecv, att, sm, blocks, wall, zs, zr, zm, rs, rr, st,
    in_sem, tok_s, tok_r, q_s, q_r, att_s, att_r, w_s, w_r,
    b_s, b_r, f_s, f_r, z_s, z_r, r_s, r_r, st_s, st_r, round_s,
):
    e = lax.axis_index("ep")
    t = lax.axis_index("tp")
    core = lax.rem(e, 2)
    chip = e // 2
    other = 1 - core
    sibling = chip * 2 + other
    n_dev = n_ep * n_tp
    nh = n_ep // 2
    n_same = nh * n_tp
    own, width = tokens_h.shape
    group = own * n_tp
    part = width // n_tp
    heads = lambdas_h.shape[0]
    heads_here = heads // n_tp
    topk = routes_h.shape[1]
    length = kc_h.shape[1]
    flat = e * n_tp + t

    barrier = pltpu.get_barrier_semaphore()
    bits = (n_dev - 1).bit_length()

    def across(k):
        step = 1 << k
        peer = flat + step * (1 - 2 * lax.rem(flat // step, 2))
        return (peer // n_tp, lax.rem(peer, n_tp))

    for k in range(bits):
        pl.semaphore_signal(barrier, inc=1, device_id=across(k), device_id_type=MESH)

    def spread(k):
        pl.semaphore_signal(round_s.at[k], inc=1, device_id=across(k), device_id_type=MESH)
        pl.semaphore_wait(round_s.at[k], 1)

    pairs = [
        (tokens_h, tok.at[t]), (lengths_h, lens), (routes_h, routes), (logits_h, logits),
        (kw_h, kw), (vw_h, vw), (qw_h, qw), (lambdas_h, lam), (hg_h, hg), (g1_h, g1), (g2_h, g2),
        (kc_h, kc), (vc_h, vc), (ow_h, ow), (gw_h.at[0], gw), (uw_h.at[0], uw), (dw_h.at[0], dw),
    ]
    loads = [pltpu.make_async_copy(a, b, in_sem.at[i]) for i, (a, b) in enumerate(pairs)]
    for load in loads:
        load.start()
    (l_tok, l_len, l_routes, l_logits, l_kw, l_vw, l_qw, l_lam, l_hg, l_g1, l_g2,
     l_kc, l_vc, l_ow, l_gw, l_uw, l_dw) = loads

    l_routes.wait()
    l_logits.wait()
    raw = logits[...]
    grown = jnp.exp(raw - jnp.max(raw, axis=1, keepdims=True))
    share = grown / jnp.sum(grown, axis=1, keepdims=True)
    named = routes[...]
    lanes = wall.shape[2]
    lane_w = lax.broadcasted_iota(jnp.int32, (group, lanes), 1)
    dense = jnp.zeros((group, lanes), F32)
    for k in range(topk):
        dense = jnp.where(named[:, k:k + 1] == lane_w, share[:, k:k + 1], dense)
    my_slot = core * nh + chip
    wall[my_slot] = dense

    l_len.wait()
    cos_g, sin_g = turns(column([lens[r].astype(F32) for r in range(group)], group), head_dim)
    own_lens = [lens[t * own + r] for r in range(own)]
    cos_o, sin_o = turns(column([v.astype(F32) for v in own_lens], own), head_dim)

    l_tok.wait()
    pl.semaphore_wait(barrier, bits)

    def swap(ref, send, recv, src_of=None):
        copies = []
        for d in range(1, n_tp):
            to = lax.rem(t + d, n_tp)
            src = ref.at[t] if src_of is None else src_of.at[to]
            copies.append(pltpu.make_async_remote_copy(
                src_ref=src, dst_ref=ref.at[t], send_sem=send.at[d - 1], recv_sem=recv.at[d - 1],
                device_id=(e, to), device_id_type=MESH,
            ))
        for copy in copies:
            copy.start()
        return copies

    tok_copies = swap(tok, tok_s, tok_r)

    def send_w(i):
        to = lax.rem(e + i + 1, n_ep)
        pltpu.make_async_remote_copy(
            src_ref=wall.at[my_slot], dst_ref=wall.at[my_slot], send_sem=w_s, recv_sem=w_r,
            device_id=(to, t), device_id_type=MESH,
        ).start()


    mine = tok[t]
    l_kw.wait()
    new_key = jnp.dot(mine, kw[...], preferred_element_type=F32)
    new_key = turn(new_key, cos_o, sin_o, head_dim).astype(BF16).astype(F32)
    l_vw.wait()
    new_value = jnp.dot(mine, vw[...], preferred_element_type=F32).astype(BF16).astype(F32)

    l_qw.wait()
    for k in range(1, min(3, bits)):
        spread(k)
    for copy in tok_copies:
        copy.wait_recv()
    for s in range(n_tp):
        tokf[s * own:(s + 1) * own, :] = tok[s].astype(F32)
    query = jnp.dot(tokf[...].astype(BF16), qw[...], preferred_element_type=F32)
    for h in range(heads_here):
        cut = slice(h * LANES, (h + 1) * LANES)
        turned = turn(query[:, cut], cos_g, sin_g, head_dim)
        for s in range(n_tp):
            qsend[s, :, cut] = turned[s * own:(s + 1) * own, :].astype(BF16)
    q_copies = swap(qrecv, q_s, q_r, qsend)
    qrecv[t] = qsend[t]
    for k in range(3, min(4, bits)):
        spread(k)

    l_lam.wait()
    l_hg.wait()
    l_kc.wait()
    l_vc.wait()
    for copy in q_copies:
        copy.wait_recv()

    scale = head_dim ** (-0.5)
    rows2 = 2 * heads
    row = lax.broadcasted_iota(jnp.int32, (rows2, LANES), 0)
    lane = lax.broadcasted_iota(jnp.int32, (rows2, LANES), 1)
    my_map = (row // heads) == (lane // head_dim)
    position = lax.broadcasted_iota(jnp.int32, (rows2, length), 1)
    mixing = column([lam[h] for h in range(heads)], heads)[:, :1]
    queries = [qrecv[s].astype(F32) for s in range(n_tp)]
    outs = []
    for b in range(own):
        qm = jnp.zeros((rows2, LANES), F32)
        for h in range(heads):
            at = (h % heads_here) * LANES
            piece = queries[h // heads_here][b:b + 1, at:at + LANES]
            qm = jnp.where(row % heads == h, piece, qm)
        qm = jnp.where(my_map, qm, 0.0)
        past = lax.dot_general(
            qm.astype(BF16), kc[b], (((1,), (1,)), ((), ())), preferred_element_type=F32
        ) * scale
        past = jnp.where(position < own_lens[b], past, -jnp.inf)
        selfs = jnp.sum(qm * new_key[b:b + 1, :], axis=1, keepdims=True) * scale
        top = jnp.maximum(jnp.max(past, axis=1, keepdims=True), selfs)
        past_exp = jnp.exp(past - top)
        self_exp = jnp.exp(selfs - top)
        total = jnp.sum(past_exp, axis=1, keepdims=True) + self_exp
        past_prob = past_exp / total
        self_prob = self_exp / total
        weight = (past_prob[:heads] - mixing * past_prob[heads:]).astype(BF16)
        self_weight = (self_prob[:heads] - mixing * self_prob[heads:]).astype(BF16).astype(F32)
        head_out = jnp.dot(weight, vc[b], preferred_element_type=F32)
        head_out = head_out + self_weight * new_value[b:b + 1, :]
        square = jnp.mean(head_out * head_out, axis=1, keepdims=True)
        outs.append(head_out * lax.rsqrt(square + EPS) * hg[...])
    row_o = lax.broadcasted_iota(jnp.int32, (own, LANES), 0)
    for h in range(heads):
        piece = jnp.zeros((own, LANES), F32)
        for b in range(own):
            piece = jnp.where(row_o == b, outs[b][h:h + 1, :], piece)
        att[t, :, h * LANES:(h + 1) * LANES] = piece.astype(BF16)
    att_copies = swap(att, att_s, att_r)
    for k in range(4, bits):
        spread(k)
    repeat(n_ep - 1, send_w)

    l_ow.wait()
    l_g1.wait()
    l_g2.wait()
    cols = pl.ds(pl.multiple_of(t * part, LANES), part)
    for copy in att_copies:
        copy.wait_recv()
    for s in range(n_tp):
        sm[s * own:(s + 1) * own, :] = att[s].astype(F32)
    mix = jnp.dot(sm[...].astype(BF16), ow[...], preferred_element_type=F32)
    summed = ALPHA * tokf[:, cols] + mix
    blocks[core, t, chip] = summed.astype(BF16)

    rank = chip * n_tp + t
    low = rank < n_same // 2

    def send_block(i):
        v = jnp.where(low, n_same - 2 - i, i)
        to = v + (v >= rank).astype(jnp.int32)
        pltpu.make_async_remote_copy(
            src_ref=blocks.at[core, t, chip], dst_ref=blocks.at[core, t, chip],
            send_sem=b_s, recv_sem=b_r.at[rank],
            device_id=(to // n_tp * 2 + core, lax.rem(to, n_tp)), device_id_type=MESH,
        ).start()

    repeat(n_same - 1, send_block)

    def forward(src):
        at = blocks.at[core, lax.rem(src, n_tp), src // n_tp]
        pltpu.make_async_remote_copy(
            src_ref=at, dst_ref=at, send_sem=f_s, recv_sem=f_r,
            device_id=(sibling, t), device_id_type=MESH,
        ).start()

    forward(rank)

    def take_block(i):
        src = lax.rem(rank - (i + 1) + n_same, n_same)
        at = blocks.at[core, lax.rem(src, n_tp), src // n_tp]
        pltpu.make_async_remote_copy(
            src_ref=at, dst_ref=at, send_sem=b_s, recv_sem=b_r.at[src],
            device_id=(sibling, t), device_id_type=MESH,
        ).wait_recv()
        forward(src)

    repeat(n_same - 1, take_block)

    def await_bytes(ref, sem):
        pltpu.make_async_copy(ref, ref, sem).wait()

    await_bytes(wall.at[pl.ds(0, n_ep - 1)], w_r)
    l_gw.wait()
    l_uw.wait()
    l_dw.wait()

    count = max(1, min(nh, 128 // group))
    rows = count * group

    def settle(pieces, gains):
        mean = sum(jnp.sum(x, axis=-1, keepdims=True) for x in pieces) / width
        pieces = [x - mean for x in pieces]
        spread = sum(jnp.sum(x * x, axis=-1, keepdims=True) for x in pieces) / width
        inverse = lax.rsqrt(spread + EPS)
        return [x * inverse * g for x, g in zip(pieces, gains)]

    gains = [g1[:, s * part:(s + 1) * part] for s in range(n_tp)]

    def expert(parity, store):
        def step(c):
            first = c * count
            pieces = [
                blocks[parity, s, pl.ds(first, count)].astype(F32).reshape(rows, part)
                for s in range(n_tp)
            ]
            x = jnp.concatenate([v.astype(BF16) for v in settle(pieces, gains)], axis=1)
            gate = jnp.dot(x, gw[...], preferred_element_type=F32)
            up = jnp.dot(x, uw[...], preferred_element_type=F32)
            clipped = jnp.minimum(gate, LIMIT)
            linear = jnp.clip(up, -LIMIT, LIMIT)
            act = (clipped * jax.nn.sigmoid(SLOPE * clipped) * (linear + 1.0)).astype(BF16)
            dense = wall[pl.ds(parity * nh + first, count)].reshape(rows, lanes)
            lane_e = lax.broadcasted_iota(jnp.int32, dense.shape, 1)
            share = jnp.sum(jnp.where(lane_e == e, dense, 0.0), axis=1, keepdims=True)
            terms = jnp.dot(act, dw[...], preferred_element_type=F32) * share
            for s in range(n_tp):
                store(s, first, terms[:, s * part:(s + 1) * part].reshape(count, group, part))

        repeat(nh // count, step)

    def store_sibling(s, first, value):
        zs[s, pl.ds(first, count)] = value.astype(BF16)

    def store_mine(s, first, value):
        zm[s, pl.ds(first, count)] = value

    expert(core, store_sibling)
    z_copy = pltpu.make_async_remote_copy(
        src_ref=zs, dst_ref=zr, send_sem=z_s, recv_sem=z_r,
        device_id=(sibling, t), device_id_type=MESH,
    )
    z_copy.start()
    await_bytes(blocks.at[other], f_r)
    expert(other, store_mine)
    z_copy.wait_recv()

    def add_chunk(c):
        at = pl.ds(c * count, count)
        for s in range(n_tp):
            rs[s, at] = (zm[s, at] + zr[s, at].astype(F32)).astype(BF16)

    repeat(nh // count, add_chunk)

    def send_result(i):
        to = jnp.where(low, n_same - 1 - i, i)
        to_chip = to // n_tp
        to_tp = lax.rem(to, n_tp)
        pltpu.make_async_remote_copy(
            src_ref=rs.at[to_tp, to_chip], dst_ref=rr.at[t, chip], send_sem=r_s, recv_sem=r_r,
            device_id=(to_chip * 2 + other, to_tp), device_id_type=MESH,
        ).start()

    repeat(n_same, send_result)

    pieces = [blocks[core, s, chip].astype(F32) for s in range(n_tp)]
    mean = sum(jnp.sum(x, axis=1, keepdims=True) for x in pieces) / width
    spread = sum(jnp.sum((x - mean) * (x - mean), axis=1, keepdims=True) for x in pieces) / width
    here = blocks[core, t, chip].astype(F32)
    settled = ((here - mean) * lax.rsqrt(spread + EPS) * g1[:, cols]).astype(BF16).astype(F32)

    await_bytes(rr, r_r)
    final = ALPHA * settled
    if n_same <= 32:
        for s in range(n_tp):
            for c in range(nh):
                final = final + rr[s, c].astype(F32)
    else:
        def add(i, total):
            return total + rr[lax.rem(i, n_tp), i // n_tp].astype(F32)

        final = lax.fori_loop(0, n_same, add, final)
    lane_s = lax.broadcasted_iota(jnp.int32, (group, LANES), 1)
    sums = jnp.sum(final, axis=1, keepdims=True)
    squares = jnp.sum(final * final, axis=1, keepdims=True)
    st[t] = jnp.where(lane_s == 0, sums, squares)
    st_copies = swap(st, st_s, st_r)
    for copy in st_copies:
        copy.wait_recv()
    stats = sum(st[s] for s in range(n_tp)) / width
    mean = stats[:, 0:1]
    spread = stats[:, 1:2] - mean * mean
    out_ref[...] = ((final - mean) * lax.rsqrt(spread + EPS) * g2[:, cols]).astype(BF16)

    for copy in tok_copies + q_copies + att_copies + st_copies + [z_copy]:
        copy.wait_send()
    await_bytes(wall.at[pl.ds(0, n_ep - 1)], w_s)
    await_bytes(rr, r_s)
    await_bytes(blocks.at[core], f_s)
    if n_tp > 1:
        await_bytes(blocks.at[core, pl.ds(0, n_tp - 1)], b_s)
    await_bytes(blocks.at[core, 0, pl.ds(0, nh - 1)], b_s)


def body(mesh_shape, *args):
    (tokens, lengths, key_cache, value_cache, query_weight, key_weight, value_weight, lambdas,
     head_gain, output_weight, norm1_gain, routes, route_logits, gate_weight, up_weight,
     down_weight, norm2_gain) = args
    n_ep, n_tp = mesh_shape
    own, width = tokens.shape
    group = own * n_tp
    part = width // n_tp
    nh = n_ep // 2
    n_same = nh * n_tp
    heads = lambdas.shape[0]
    value_dim = value_weight.shape[1]
    head_dim = key_weight.shape[1] // 2
    lanes = -(-n_ep // LANES) * LANES
    operands = (
        tokens, lengths, key_cache, value_cache, query_weight, key_weight, value_weight, lambdas,
        head_gain.reshape(1, -1), output_weight, norm1_gain.reshape(1, -1), routes, route_logits,
        gate_weight, up_weight, down_weight, norm2_gain.reshape(1, -1),
    )
    v = pltpu.VMEM
    dma = pltpu.SemaphoreType.DMA
    partners = max(1, n_tp - 1)
    scratch = [
        v((n_tp, own, width), BF16), pltpu.SMEM(lengths.shape, jnp.int32),
        v(key_cache.shape, BF16), v(value_cache.shape, BF16), v(query_weight.shape, BF16),
        v(key_weight.shape, BF16), v(value_weight.shape, BF16), pltpu.SMEM(lambdas.shape, F32),
        v((1, value_dim), F32), v(output_weight.shape, BF16), v((1, width), F32),
        v(routes.shape, jnp.int32), v(route_logits.shape, F32), v(gate_weight.shape[1:], BF16),
        v(up_weight.shape[1:], BF16), v(down_weight.shape[1:], BF16), v((1, width), F32),
        v((group, width), F32),
        v((n_tp, own, query_weight.shape[1]), BF16), v((n_tp, own, query_weight.shape[1]), BF16),
        v((n_tp, own, heads * value_dim), BF16), v((group, heads * value_dim), F32),
        v((2, n_tp, nh, group, part), BF16), v((n_ep, group, lanes), F32),
        v((n_tp, nh, group, part), BF16), v((n_tp, nh, group, part), BF16),
        v((n_tp, nh, group, part), F32), v((n_tp, nh, group, part), BF16),
        v((n_tp, nh, group, part), BF16), v((n_tp, group, LANES), F32),
        dma((len(operands),)), dma((partners,)), dma((partners,)), dma((partners,)),
        dma((partners,)), dma((partners,)), dma((partners,)), dma, dma,
        dma, dma((n_same,)), dma, dma, dma, dma, dma, dma, dma((partners,)), dma((partners,)),
        pltpu.SemaphoreType.REGULAR(((n_ep * n_tp).bit_length(),)),
    ]
    return pl.pallas_call(
        functools.partial(kernel, n_ep, n_tp, head_dim),
        out_shape=pltpu.VMEM((group, part), BF16),
        in_specs=[pl.BlockSpec(memory_space=pl.ANY)] * len(operands),
        out_specs=pl.BlockSpec(memory_space=pltpu.VMEM),
        scratch_shapes=scratch,
        compiler_params=pltpu.CompilerParams(
            collective_id=0, has_side_effects=True, vmem_limit_bytes=60 * 1024 * 1024
        ),
    )(*operands)


def solution(mesh):
    in_specs = (
        P(("ep", "tp"), None),
        P("ep"),
        P(("ep", "tp"), None, None),
        P(("ep", "tp"), None, None),
        P(None, "tp"),
        P(),
        P(),
        P(),
        P(),
        P(None, "tp"),
        P(),
        P("ep", None),
        P("ep", None),
        P("ep", None, "tp"),
        P("ep", None, "tp"),
        P("ep", "tp", None),
        P(),
    )
    out_specs = P("ep", "tp")
    shape = (mesh.shape["ep"], mesh.shape["tp"])
    return jax.shard_map(
        functools.partial(body, shape), mesh=mesh, in_specs=in_specs, out_specs=out_specs,
        check_vma=False,
    )
```
